256 devices in a mesh: ep: 16 (over y, x), tp: 16 (over z, core).
Axes of the slice: x: 4, y: 4, z: 8, core: 2. Of those that a mesh axis runs over, the one named last changes fastest.
Arguments:
- query_latent: bfloat16 [8192, 1024], P('ep'), may hold values from -6 to 6
- joint_latent: bfloat16 [8192, 512], P('ep'), may hold values from -6 to 6
- rotary_key: bfloat16 [8192, 32], P('ep'), may hold values from -60 to 60
- query_gain: float32 [1024], replicated, may hold values from 0.1 to 1.9
- joint_gain: float32 [512], replicated, may hold values from 0.1 to 1.9
- query_weight: bfloat16 [1024, 2048], P(None, 'tp'), may hold values from -0.1875 to 0.1875
- query_rotary: bfloat16 [1024, 1024], P(None, 'tp'), may hold values from -0.1875 to 0.1875
- key_weight: bfloat16 [512, 2048], P(None, 'tp'), may hold values from -0.25 to 0.25
- value_weight: bfloat16 [512, 2048], P(None, 'tp'), may hold values from -0.25 to 0.25
- output_weight: bfloat16 [2048, 2048], P('tp'), may hold values from -6 to 6
- expert_input: bfloat16 [8192, 2048], P('ep'), may hold values from -6 to 6
- expert_gain: float32 [2048], replicated, may hold values from 0.1 to 1.9
- routes: int32 [8192, 2], P('ep'), may hold values from 0 to 31, all different within a row; in each aligned block of 512 rows (0 to 511, 512 to 1023, ...) at most 48 rows name the same one
- route_weight: float32 [8192, 2], P('ep'), may hold values from 0.2 to 1
- gate_weight: bfloat16 [32, 2048, 4096], P('ep', None, 'tp'), may hold values from -0.125 to 0.125
- up_weight: bfloat16 [32, 2048, 4096], P('ep', None, 'tp'), may hold values from -0.125 to 0.125
- down_weight: bfloat16 [32, 4096, 2048], P('ep', 'tp'), may hold values from -0.09375 to 0.09375
Outputs:
- mixer_out: bfloat16 [8192, 2048], P(('ep', 'tp'))
- expert_out: bfloat16 [8192, 2048], P('ep', 'tp')
The draws below stay inside these ranges and needn't reach their ends.
Inputs may be any that keep to these rules, and one draw needn't show every extreme that they name: `routes`: A row names 2 different experts. Among the rows of one device (aligned blocks of 512 rows) no expert is named by more than 48 rows, a bound that some block reaches.
All inputs are finite; a program needn't handle non-finite values.
Results may differ from the reference program's by a relative error of at most 0.019.
The reference program's roundings to bfloat16 on the way count: a program that leaves them out, or rounds other values in their place, can miss the bound.
Values may be sent and summed in bfloat16 or wider, within the bound.
A program may use at most 128 MiB of HBM per device.

```python
import math
import jax
import jax.numpy as jnp
import numpy as np
from jax import lax

D = 2048
HEADS = 32
NOPE = 64
ROPE = 32
VDIM = 64
QL = 1024
KVL = 512
FF = 4096
TOPK = 2
TOK_B_DEV = 512
EXPERTS = 32
TOK_A = 8192
TOK_B = 8192
CAP = 48
N_EP = 16
N_TP = 16


def draw_rotary_key(key, part):
    base = jax.random.normal(jax.random.fold_in(key, 11), (TOK_A, ROPE), jnp.float32)
    return jnp.clip(base, -60.0, 60.0).astype(jnp.bfloat16)


def level_of(stream_key, shape, shards, low, high):
    def one(dim, blocks):
        draws = jax.random.uniform(jax.random.fold_in(jax.random.fold_in(stream_key, 6), dim), (blocks,), jnp.float32, low / len(shards), high / len(shards))
        return jnp.repeat(jnp.exp(draws), shape[dim] // blocks).reshape((-1,) + (1,) * (len(shape) - dim - 1))

    gain = one(*shards[0])
    for cut in shards[1:]:
        gain = gain * one(*cut)
    return gain


def deal_out(rng, own, number, rows, amount, top, most, slope):
    sequence = jax.random.permutation(rng, amount)
    packed, usual = load_shares(amount, rows * top, most, slope, True), load_shares(amount, rows * top, most, slope, False)
    places = jnp.arange(amount)

    def named(sizes, rotation):
        used = int((sizes > 0).sum())
        fixed = max(1, used // 4)
        passed = fixed + (places - fixed + rotation * (used - fixed)) % max(1, amount - fixed)
        return jnp.zeros((amount,), jnp.int32).at[sequence[jnp.where(places < fixed, places, passed)]].set(jnp.asarray(sizes, jnp.int32))

    sizes = jnp.where(number % 4 == 0, named(packed, number // 4), named(usual, number - number // 4 - 1))
    mixed = jax.random.permutation(jax.random.fold_in(own, 3), amount)
    giver, receiver = mixed[0:amount // 2 * 2:2], mixed[1:amount // 2 * 2:2]
    margin = jnp.minimum(sizes[giver] - 1, most - sizes[receiver]) // 2
    margin = jnp.where((giver == sequence[0]) | (receiver == sequence[0]) | (sizes[receiver] == 0), 0, jnp.maximum(margin, 0))
    passed = jax.random.randint(jax.random.fold_in(own, 4), (amount // 2,), 0, 1 << 20) % (margin + 1)
    sizes = sizes.at[giver].add(-passed).at[receiver].add(passed)
    members = jnp.searchsorted(jnp.cumsum(sizes), jnp.arange(rows * top), side="right").astype(jnp.int32)
    listing = members.reshape(top, rows).T
    listing = listing[jax.random.permutation(jax.random.fold_in(own, 1), rows)]
    rotation = jax.random.randint(jax.random.fold_in(own, 2), (rows, 1), 0, top)
    return jnp.take_along_axis(listing, (jnp.arange(top)[None, :] + rotation) % top, axis=1)


def load_shares(count, total, reach, skew, full):
    weights = [(1 << 20) // math.isqrt(grade ** skew) + 1 for grade in range(1, count + 1)]
    largest = reach if full else min(reach, max(-(-total // count), total * weights[0] // sum(weights)))
    least = 1 if total - largest >= count - 1 else 0
    given, rest = [largest] + [least] * (count - 1), total - largest - least * (count - 1)
    while rest > 0:
        free = [i for i in range(1, count) if given[i] < largest] or [i for i in range(1, count) if given[i] < reach]
        mass, remaining = sum([weights[i] for i in free]), rest
        for i in free:
            addition = min(reach - given[i], max(1, remaining * weights[i] // mass), rest)
            given[i] = given[i] + addition
            rest = rest - addition
    return np.array(given)


def gaussian(stream_key, dims, scale, bound, cuts=(), kind=jnp.bfloat16):
    loudness = level_of(stream_key, dims, cuts, -0.22, 0.18) if cuts else 1.0
    result = jax.random.normal(stream_key, dims, jnp.float32) * scale * loudness
    return jnp.minimum(jnp.maximum(result, -bound), bound).astype(kind)


def setup_inputs(seed: int = 0) -> dict:
    keys = jax.random.split(jax.random.key(seed), 18)
    query_latent = gaussian(keys[0], (TOK_A, QL), 1.0, 6.0, ((0, 16),))
    joint_latent = gaussian(keys[1], (TOK_A, KVL), 1.0, 6.0, ((0, 16),))
    rotary_key = draw_rotary_key(jax.random.fold_in(keys[17], 71), 0)
    query_gain = jnp.clip(1.0 + 0.18 * jax.random.normal(keys[3], (QL,), jnp.float32), 0.1, 1.9)
    joint_gain = jnp.clip(1.0 + 0.18 * jax.random.normal(keys[4], (KVL,), jnp.float32), 0.1, 1.9)
    query_weight = gaussian(keys[5], (QL, HEADS * NOPE), QL ** -0.5, 0.1875, ((1, 16),))
    query_rotary = gaussian(keys[6], (QL, HEADS * ROPE), QL ** -0.5, 0.1875, ((1, 16),))
    key_weight = gaussian(keys[7], (KVL, HEADS * NOPE), KVL ** -0.5, 0.25, ((1, 16),))
    value_weight = gaussian(keys[8], (KVL, HEADS * VDIM), KVL ** -0.5, 0.25, ((1, 16),))
    output_weight = gaussian(keys[9], (HEADS * VDIM, D), 1.0, 6.0, ((0, 16),))
    expert_input = gaussian(keys[10], (TOK_B, D), 1.0, 6.0, ((0, 16),))
    expert_gain = jnp.clip(1.0 + 0.18 * jax.random.normal(keys[11], (D,), jnp.float32), 0.1, 1.9)
    routes_keys = jax.random.split(jax.random.fold_in(keys[12], 1), TOK_B // TOK_B_DEV)
    routes_turns = jax.random.permutation(jax.random.fold_in(keys[12], 3), TOK_B // TOK_B_DEV)
    routes = jax.vmap(lambda own, number: deal_out(jax.random.fold_in(keys[12], 2), own, number, TOK_B_DEV, EXPERTS, TOPK, CAP, 1))(routes_keys, routes_turns).reshape((TOK_B, TOPK))
    route_weight = jnp.clip(0.2 + 0.8 * jax.random.uniform(keys[13], (TOK_B, TOPK), jnp.float32) ** level_of(keys[13], (TOK_B, TOPK), ((0, 16),), -0.2, 0.2), 0.2, 1.0)
    gate_weight = gaussian(keys[14], (EXPERTS, D, FF), D ** -0.5, 0.125, ((0, 16), (2, 16)))
    up_weight = gaussian(keys[15], (EXPERTS, D, FF), D ** -0.5, 0.125, ((0, 16), (2, 16)))
    down_weight = gaussian(keys[16], (EXPERTS, FF, D), FF ** -0.5, 0.09375, ((0, 16), (1, 16)))
    return dict(query_latent=query_latent, joint_latent=joint_latent, rotary_key=rotary_key, query_gain=query_gain, joint_gain=joint_gain, query_weight=query_weight, query_rotary=query_rotary, key_weight=key_weight, value_weight=value_weight, output_weight=output_weight, expert_input=expert_input, expert_gain=expert_gain, routes=routes, route_weight=route_weight, gate_weight=gate_weight, up_weight=up_weight, down_weight=down_weight)


NORM_EPSILON = 1e-06
ROTARY_BASE = 10000.0

def norm_rows(source, gain_vector):
    as_float = source.astype(jnp.float32)
    factor = lax.rsqrt(lax.optimization_barrier(jnp.mean(as_float * as_float, axis=-1, keepdims=True)) + NORM_EPSILON)
    return (as_float * factor * gain_vector.astype(jnp.float32)).astype(jnp.bfloat16)

def rotate(source, positions):
    half_width = source.shape[-1] // 2
    frequencies = ROTARY_BASE ** (-jnp.arange(half_width, dtype=jnp.float32) / half_width)
    angles = positions[:, None] * frequencies[None, :]
    view_shape = (source.shape[0],) + (1,) * (source.ndim - 2) + (half_width,)
    cosine_table = jnp.cos(angles).reshape(view_shape)
    sine_table = jnp.sin(angles).reshape(view_shape)
    first_half = source[..., :half_width]
    second = source[..., half_width:]
    return jnp.concatenate([first_half * cosine_table - second * sine_table, second * cosine_table + first_half * sine_table], axis=-1)

def reference(query_latent, joint_latent, rotary_key, query_gain, joint_gain, query_weight, query_rotary, key_weight, value_weight, output_weight, expert_input, expert_gain, routes, route_weight, gate_weight, up_weight, down_weight):
    positions = jnp.arange(TOK_A, dtype=jnp.float32)
    query_normed = norm_rows(query_latent, query_gain)
    joint_normed = norm_rows(joint_latent, joint_gain)
    turned_key = rotate(rotary_key.astype(jnp.float32), positions).astype(jnp.bfloat16)
    query_plain = jnp.dot(query_normed, query_weight, preferred_element_type=jnp.float32).astype(jnp.bfloat16)
    query_plain = query_plain.reshape(TOK_A, HEADS, NOPE)
    query_turned = jnp.dot(query_normed, query_rotary, preferred_element_type=jnp.float32)
    query_turned = rotate(query_turned.reshape(TOK_A, HEADS, ROPE), positions).astype(jnp.bfloat16)
    key_plain = jnp.dot(joint_normed, key_weight, preferred_element_type=jnp.float32).astype(jnp.bfloat16)
    key_plain = key_plain.reshape(TOK_A, HEADS, NOPE)
    values = jnp.dot(joint_normed, value_weight, preferred_element_type=jnp.float32).astype(jnp.bfloat16)
    values = values.reshape(TOK_A, HEADS, VDIM)
    score_scale = (NOPE + ROPE) ** (-0.5)

    def one_head(items_in):
        query_head, turned_head, key_head, value_head = items_in
        scores = jnp.dot(query_head, key_head.T, preferred_element_type=jnp.float32)
        scores = (scores + jnp.dot(turned_head, turned_key.T, preferred_element_type=jnp.float32)) * score_scale
        row_top = lax.optimization_barrier(jnp.max(scores, axis=-1, keepdims=True))
        expo = jnp.exp(scores - row_top)
        row_total = lax.optimization_barrier(jnp.sum(expo, axis=-1, keepdims=True))
        mixed_values = jnp.dot(expo.astype(jnp.bfloat16), value_head, preferred_element_type=jnp.float32)
        return (mixed_values / row_total).astype(jnp.bfloat16)
    per_head = lax.map(one_head, (query_plain.transpose(1, 0, 2), query_turned.transpose(1, 0, 2), key_plain.transpose(1, 0, 2), values.transpose(1, 0, 2)))
    attended = per_head.transpose(1, 0, 2).reshape(TOK_A, HEADS * VDIM)
    mixer_out = jnp.dot(attended, output_weight, preferred_element_type=jnp.float32).astype(jnp.bfloat16)
    expert_normed = norm_rows(expert_input, expert_gain)
    flat_routes = routes.reshape(-1).astype(jnp.int32)
    pair_count = TOK_B * TOPK
    owner_token = jnp.arange(pair_count, dtype=jnp.int32) // TOPK
    onehot = (flat_routes[:, None] == jnp.arange(EXPERTS, dtype=jnp.int32)[None, :]).astype(jnp.int32)
    rank_within = lax.optimization_barrier(jnp.sum((jnp.cumsum(onehot, axis=0) - onehot) * onehot, axis=1)).astype(jnp.int32)
    slot_width = N_EP * CAP
    slot_token = jnp.zeros((EXPERTS, slot_width), jnp.int32).at[flat_routes, rank_within].set(owner_token)
    block_width = FF // N_TP

    def one_expert(items_in):
        token_index, gate_matrix, up_matrix, down_matrix = items_in
        rows_in = expert_normed[token_index]
        gate_acts = jnp.dot(rows_in, gate_matrix, preferred_element_type=jnp.float32)
        up_acts = jnp.dot(rows_in, up_matrix, preferred_element_type=jnp.float32)
        hidden = (jax.nn.silu(gate_acts) * up_acts).astype(jnp.bfloat16)

        def add_block(running, block_index):
            start_at = (block_index * block_width).astype(jnp.int32)
            part_sum = jnp.dot(lax.dynamic_slice_in_dim(hidden, start_at, block_width, 1), lax.dynamic_slice_in_dim(down_matrix, start_at, block_width, 0), preferred_element_type=jnp.float32)
            part_sum = lax.optimization_barrier(part_sum.astype(jnp.bfloat16))
            return (running + part_sum.astype(jnp.float32), None)
        running, _ = lax.scan(add_block, jnp.zeros((slot_width, D), jnp.float32), jnp.arange(N_TP, dtype=jnp.int32))
        return running.astype(jnp.bfloat16)
    results = lax.map(one_expert, (slot_token, gate_weight, up_weight, down_weight))
    picked = results[flat_routes, rank_within].astype(jnp.float32).reshape(TOK_B, TOPK, D)
    expert_out = lax.optimization_barrier(jnp.sum(picked * route_weight[:, :, None], axis=1)).astype(jnp.bfloat16)
    return (mixer_out, expert_out)
```

```python
import functools

import jax
import jax.numpy as jnp
from jax import lax
from jax.experimental import pallas as pl
from jax.experimental.pallas import tpu as pltpu
from jax.sharding import PartitionSpec as P

NOPE = 64
VDIM = 64
ROPE = 32
NORM_EPSILON = 1e-06
ROTARY_BASE = 10000.0
LANES = 128
LOG2E = 1.4426950408889634
MESH = pl.DeviceIdType.MESH
F32 = jnp.float32
BF16 = jnp.bfloat16


def ep_grid(count):
    return {16: (4, 4), 4: (2, 2), 2: (1, 2)}[count]


def dot(a, b):
    return jnp.dot(a, b, preferred_element_type=F32)


def dot_nt(a, b):
    return lax.dot_general(a, b, (((1,), (1,)), ((), ())), preferred_element_type=F32)


def front_kernel(
    cap, experts, ql, jl, rk_t, qgain, jgain, wa, wb, cq, sq, wk_t, wv, xin, egain, routes, routes_t,
    slots_out, kt_out, v_out, q_out, slot_out,
):
    tokens = ql.shape[0]
    half = tokens // 2

    def normed(ref, gain):
        x = ref[...].astype(F32)
        factor = lax.rsqrt(jnp.mean(x * x, axis=-1, keepdims=True) + NORM_EPSILON)
        return (x * factor * gain[...]).astype(BF16)

    r = routes[...]
    rt = routes_t[...]
    row = lax.broadcasted_iota(jnp.int32, (tokens, tokens), 0)
    col = lax.broadcasted_iota(jnp.int32, (tokens, tokens), 1)
    lane_e = lax.broadcasted_iota(jnp.int32, (tokens, experts), 1)
    named0 = lane_e == r[:, 0:1]
    named1 = lane_e == r[:, 1:2]
    named = (named0 | named1).astype(F32).astype(BF16)
    before = dot((col < row).astype(F32).astype(BF16), named)
    place = before.astype(jnp.int32) + lane_e * cap
    slot0 = jnp.sum(jnp.where(named0, place, 0), axis=1, keepdims=True)
    slot1 = jnp.sum(jnp.where(named1, place, 0), axis=1, keepdims=True)
    slot_out[...] = jnp.concatenate([slot0, slot1], axis=1)

    sub_e = lax.broadcasted_iota(jnp.int32, (experts, tokens), 0)
    named_t = (sub_e == rt[0:1, :]) | (sub_e == rt[1:2, :])
    before_t = dot(named_t.astype(F32).astype(BF16), (row < col).astype(F32).astype(BF16))
    rank_t = jnp.where(named_t, before_t, -1.0)

    x = xin[...].astype(F32)
    factor = lax.rsqrt(jnp.mean(x * x, axis=-1, keepdims=True) + NORM_EPSILON)
    at = pl.multiple_of(lax.axis_index("tp") * LANES, LANES)
    mine = (xin[:, pl.ds(at, LANES)].astype(F32) * factor * egain[:, pl.ds(at, LANES)]).astype(BF16)
    place_in = lax.broadcasted_iota(jnp.int32, (cap, tokens), 0).astype(F32)
    for e in range(experts):
        pick = (place_in == rank_t[e : e + 1, :]).astype(F32).astype(BF16)
        slots_out[e] = dot(pick, mine).astype(BF16)

    jn = normed(jl, jgain)
    kt = dot_nt(wk_t[...], jn).astype(BF16)
    rkt = rk_t[...]
    vv = dot(jn, wv[...]).astype(BF16)
    for h in range(2):
        part = slice(h * half, (h + 1) * half)
        kt_out[h, 0:NOPE, :] = kt[0:NOPE, part]
        kt_out[h, NOPE : NOPE + ROPE, :] = rkt[:, part]
        kt_out[h, NOPE + ROPE :, :] = kt[NOPE:, part]
        v_out[h] = vv[part]

    qn = normed(ql, qgain)
    q_out[...] = (dot(qn, wa[...]) * cq[...] + dot(qn, wb[...]) * sq[...]).astype(BF16)


def main_kernel(
    dims, slots, kt_own, v_own, q_ref, slot_ref, rw_ref, wg_hbm, wu_hbm, wd_hbm, wo_ref,
    mixer_ref, expert_ref,
    xbuf, pbuf, sbuf, rbuf, tbuf, fin, ret, ktb, vb, wg, wu, wd, m_s, l_s, acc_s,
    ap, asb, arb, atb,
    a2a_s, a2a_r, zs, zr, dds, ddr, kvs, kvr, pss, psr, rss, rsr, bks, bkr, aps, apr, ars, arr, local_s,
):
    ny, nx, nz, cap = dims
    ep_n = ny * nx
    rows = ep_n * cap
    ep = lax.axis_index("ep")
    tp = lax.axis_index("tp")
    y, x = ep // nx, lax.rem(ep, nx)
    z, c = tp // 2, lax.rem(tp, 2)
    oc = 1 - c
    sib = z * 2 + oc
    zright = lax.rem(z + 1, nz)
    zleft = lax.rem(z + nz - 1, nz)
    pending = []

    def send(src, dst, ssem, rsem, to):
        d = pltpu.make_async_remote_copy(
            src_ref=src, dst_ref=dst, send_sem=ssem, recv_sem=rsem, device_id=to, device_id_type=MESH
        )
        d.start()
        pending.append(d)

    def arrived(dst, ssem, rsem, frm):
        pltpu.make_async_remote_copy(
            src_ref=dst, dst_ref=dst, send_sem=ssem, recv_sem=rsem, device_id=frm, device_id_type=MESH
        ).wait_recv()

    own = [
        pltpu.make_async_copy(wg_hbm, wg, local_s.at[0]),
        pltpu.make_async_copy(wu_hbm, wu, local_s.at[1]),
        pltpu.make_async_copy(wd_hbm, wd, local_s.at[2]),
        pltpu.make_async_copy(slots.at[ep], xbuf.at[:, z, c, pl.ds(pl.multiple_of(ep * cap, 16), cap)], local_s.at[3]),
        pltpu.make_async_copy(kt_own.at[0], ktb.at[0, y, x], local_s.at[4]),
        pltpu.make_async_copy(kt_own.at[1], ktb.at[1, x, y], local_s.at[5]),
        pltpu.make_async_copy(v_own.at[0], vb.at[0, y, x], local_s.at[6]),
        pltpu.make_async_copy(v_own.at[1], vb.at[1, x, y], local_s.at[7]),
    ]
    for d in own[3:] + own[:3]:
        d.start()

    barrier = pltpu.get_barrier_semaphore()
    peers = [(lax.rem(ep + k, ep_n), tp) for k in range(1, ep_n)]
    peers.append((ep, sib))
    peers.append((ep, zright * 2 + c))
    if nz > 2:
        peers.append((ep, zleft * 2 + c))
    for peer in peers:
        pl.semaphore_signal(barrier, inc=1, device_id=peer, device_id_type=MESH)
    pl.semaphore_wait(barrier, len(peers))

    mine = pl.ds(pl.multiple_of(ep * cap, 16), cap)
    for k in range(1, ep_n):
        to = lax.rem(ep + k, ep_n)
        send(slots.at[to], xbuf.at[:, z, c, mine], a2a_s.at[k], a2a_r.at[k], (to, tp))

    axes = (("x", nx, x), ("y", ny, y))

    def ring_to(name, step):
        if name == "x":
            return (y * nx + lax.rem(x + nx + step, nx), tp)
        return (lax.rem(y + ny + step, ny) * nx + x, tp)

    def kv_refs(part, phase, block):
        other = (y, x)[part]
        if phase == 0:
            return ktb.at[part, other, block], vb.at[part, other, block]
        return ktb.at[part, block], vb.at[part, block]

    def kv_send(part, phase, step):
        name, n, me = axes[(part + phase) % 2]
        if n == 1 or step > n // 2:
            return
        tie = 2 * step == n
        for d, sign in ((0, 1), (1, -1)):
            block = lax.rem(me + n - sign * (step - 1), n)
            refs = kv_refs(part, phase, block)
            for kind in (0, 1):
                if not tie or kind == d:
                    i = (part, phase, d, step - 1, kind)
                    send(refs[kind], refs[kind], kvs.at[i], kvr.at[i], ring_to(name, sign))

    def kv_wait(part, phase, step):
        name, n, me = axes[(part + phase) % 2]
        if n == 1 or step > n // 2:
            return
        tie = 2 * step == n
        for d, sign in ((0, 1), (1, -1)):
            block = lax.rem(me + n - sign * step, n)
            refs = kv_refs(part, phase, block)
            for kind in (0, 1):
                if not tie or kind == d:
                    i = (part, phase, d, step - 1, kind)
                    arrived(refs[kind], kvs.at[i], kvr.at[i], ring_to(name, -sign))

    for i in (4, 5, 6, 7):
        own[i].wait()
    for part in (0, 1):
        kv_send(part, 0, 1)

    own[3].wait()
    for k in range(1, ep_n):
        frm = lax.rem(ep + ep_n - k, ep_n)
        there = xbuf.at[:, z, c, pl.ds(pl.multiple_of(frm * cap, 16), cap)]
        arrived(there, a2a_s.at[k], a2a_r.at[k], (frm, tp))

    hz = nz // 2
    hr = rows // 2
    z_to = ((ep, zright * 2 + c), (ep, zleft * 2 + c))

    def z_piece(e, block, core, d, step):
        if 2 * step == nz:
            return xbuf.at[e, block, core, pl.ds(d * hr, hr)]
        return xbuf.at[e, block, core]

    def z_send(e, step):
        for d, sign in ((0, 1), (1, -1)):
            block = lax.rem(z + nz - sign * (step - 1), nz)
            piece = z_piece(e, block, c, d, step)
            send(piece, piece, zs.at[e, d, step - 1], zr.at[e, d, step - 1], z_to[d])

    def z_wait(e, step):
        for d, sign in ((0, 1), (1, -1)):
            block = lax.rem(z + nz - sign * step, nz)
            piece = z_piece(e, block, c, d, step)
            arrived(piece, zs.at[e, d, step - 1], zr.at[e, d, step - 1], z_to[1 - d])
            if step < hz:
                after = lax.rem(z + nz - sign * step, nz)
                nxt = z_piece(e, after, c, d, step + 1)
                send(nxt, nxt, zs.at[e, d, step], zr.at[e, d, step], z_to[d])
            send(piece, piece, dds.at[e, d, step], ddr.at[e, d, step], (ep, sib))

    def dd_wait(e):
        there = xbuf.at[e, z, oc]
        arrived(there, dds.at[e, 0, 0], ddr.at[e, 0, 0], (ep, sib))
        for step in range(1, hz + 1):
            for d, sign in ((0, 1), (1, -1)):
                block = lax.rem(z + nz - sign * step, nz)
                piece = z_piece(e, block, oc, d, step)
                arrived(piece, dds.at[e, d, step], ddr.at[e, d, step], (ep, sib))

    for e in (0, 1):
        z_send(e, 1)
        piece = xbuf.at[e, z, c]
        send(piece, piece, dds.at[e, 0, 0], ddr.at[e, 0, 0], (ep, sib))

    scale = LOG2E * (NOPE + ROPE) ** (-0.5)
    tokens = q_ref.shape[0]
    q_tile = min(256, tokens)
    m_s[...] = jnp.full(m_s.shape, -jnp.inf, F32)
    l_s[...] = jnp.zeros(l_s.shape, F32)
    acc_s[...] = jnp.zeros(acc_s.shape, F32)

    def unit(part, a):
        blocks = (nx, ny)[part]

        def tile(t, carry):
            at = pl.ds(pl.multiple_of(t * q_tile, q_tile), q_tile)
            for head in (0, 1):
                q = q_ref[at, head * LANES : (head + 1) * LANES]
                s = jnp.concatenate(
                    [dot(q, ktb[part, a, b, head * ROPE : head * ROPE + LANES, :]) for b in range(blocks)], axis=1
                )
                m_old = m_s[head, at]
                m_new = jnp.maximum(m_old, jnp.max(s, axis=1, keepdims=True))
                alpha = jnp.exp2((m_old - m_new) * scale)
                p = jnp.exp2(s * scale - m_new[:, 0:1] * scale)
                l_s[head, at] = l_s[head, at] * alpha + jnp.sum(p, axis=1, keepdims=True)
                m_s[head, at] = m_new
                vals = jnp.concatenate([vb[part, a, b] for b in range(blocks)], axis=0)
                acc_s[head, at] = acc_s[head, at] * alpha + dot(p.astype(BF16), vals)
            return carry

        lax.fori_loop(0, tokens // q_tile, tile, 0)

    def kv_both(phase, step, then_phase, then_step):
        for part in (0, 1):
            kv_wait(part, phase, step)
            if then_phase is not None:
                kv_send(part, then_phase, then_step)

    kv_both(0, 1, 0, 2)
    kv_both(0, 2, 1, 1)
    for step in range(1, hz + 1):
        for e in (0, 1):
            if step == hz and e == 0:
                for i in (0, 1, 2):
                    own[i].wait()
            z_wait(e, step)
        if step == max(1, hz - 1):
            kv_both(1, 1, 1, 2)

    row_tile = 256 if rows % 256 == 0 else rows // 2
    f_width = wg.shape[2]

    def expert(e):
        dd_wait(e)

        def tile(t, carry):
            at = pl.ds(pl.multiple_of(t * row_tile, row_tile), row_tile)
            xx = jnp.concatenate([xbuf[e, i // 2, i % 2, at] for i in range(2 * nz)], axis=1)
            gate = dot(xx, wg[e])
            up = dot(xx, wu[e])
            hidden = (gate / (1.0 + jnp.exp(-gate)) * up).astype(BF16)
            part = dot(hidden, wd[e]).astype(BF16)
            for i in range(2 * nz):
                pbuf[e, i // 2, i % 2, at] = part[:, i * LANES : (i + 1) * LANES]
            return carry

        lax.fori_loop(0, rows // row_tile, tile, 0)
        send(pbuf.at[e, :, oc], sbuf.at[e], pss.at[e], psr.at[e], (ep, sib))

    def reducer(p, s, r, t, ssem, rsem):
        whole = p.shape[2]
        cut = whole // 2

        def term(dest, at):
            return p[dest, c, at].astype(F32) + s[dest, at].astype(F32)

        def put(step):
            for d, sign in ((0, 1), (1, -1)):
                dest = lax.rem(z + sign * (hz + 1 - step) + nz, nz)
                if step == 1:
                    at = pl.ds(d * cut, cut)
                    t[d, 0, at] = term(dest, at).astype(BF16)
                    piece, there = t.at[d, 0, at], r.at[d, 0, at]
                else:
                    for g in (0, 1):
                        at = pl.ds(g * cut, cut)
                        v = term(dest, at)
                        if step > 2 or g == d:
                            v = v + r[d, step - 2, at].astype(F32)
                        t[d, step - 1, at] = v.astype(BF16)
                    piece, there = t.at[d, step - 1], r.at[d, step - 1]
                send(piece, there, ssem.at[d, step - 1], rsem.at[d, step - 1], z_to[d])

        def take(step):
            for d in (0, 1):
                there = r.at[d, step - 1, pl.ds(d * cut, cut)] if step == 1 else r.at[d, step - 1]
                arrived(there, ssem.at[d, step - 1], rsem.at[d, step - 1], z_to[1 - d])

        def last():
            out = []
            for g in (0, 1):
                at = pl.ds(g * cut, cut)
                v = term(z, at)
                for d in (0, 1):
                    if hz > 1 or g == d:
                        v = v + r[d, hz - 1, at].astype(F32)
                out.append(v.astype(BF16))
            return out

        return put, take, last

    def finish(e, last):
        for g, v in enumerate(last()):
            fin[e, g * hr : (g + 1) * hr] = v
        for k in range(1, ep_n):
            to = lax.rem(ep + k, ep_n)
            src = fin.at[e, pl.ds(pl.multiple_of(to * cap, 16), cap)]
            send(src, ret.at[2 * ep + e], bks.at[e, k], bkr.at[e, k], (to, tp))
        ret[2 * ep + e] = fin[e, mine]

    a0 = (y, x)
    alen = (ny, nx)
    order = [(part, i) for i in range(max(ny, nx)) for part in (0, 1) if i < alen[part]]
    todo = list(order)

    def some(count=1):
        for _ in range(count):
            if todo:
                part, i = todo.pop(0)
                off = (i + 1) // 2 if i % 2 else alen[part] - i // 2
                unit(part, lax.rem(a0[part] + off, alen[part]))

    expert(0)
    expert(1)
    kv_both(1, 2, None, None)
    red = [
        reducer(pbuf.at[e], sbuf.at[e], rbuf.at[e], tbuf.at[e], rss.at[e], rsr.at[e]) for e in (0, 1)
    ]
    for e in (0, 1):
        arrived(sbuf.at[e], pss.at[e], psr.at[e], (ep, sib))
        red[e][0](1)
    for step in range(1, hz + 1):
        for e in (0, 1):
            some()
            red[e][1](step)
            if step < hz:
                red[e][0](step + 1)
            else:
                finish(e, red[e][2])
    some(len(todo))

    lane = lax.broadcasted_iota(jnp.int32, (tokens, LANES), 1)
    attended = jnp.where(lane < VDIM, acc_s[0] / l_s[0], acc_s[1] / l_s[1]).astype(BF16)
    proj = dot(attended, wo_ref[...]).astype(BF16)
    per = tokens // (2 * nz)
    for i in range(2 * nz):
        ap[i // 2, i % 2] = proj[i * per : (i + 1) * per]
    send(ap.at[:, oc], asb, aps, apr, (ep, sib))
    put, take, last = reducer(ap, asb, arb, atb, ars, arr)
    arrived(asb, aps, apr, (ep, sib))
    put(1)
    for step in range(1, hz + 1):
        take(step)
        if step < hz:
            put(step + 1)
    for g, v in enumerate(last()):
        mixer_ref[g * (per // 2) : (g + 1) * (per // 2)] = v

    for e in (0, 1):
        for k in range(1, ep_n):
            frm = lax.rem(ep + ep_n - k, ep_n)
            arrived(ret.at[2 * frm + e], bks.at[e, k], bkr.at[e, k], (frm, tp))
    slot_count = 2 * ep_n * cap
    where_at = lax.broadcasted_iota(jnp.int32, (tokens, slot_count), 1)
    rets = ret[...].reshape(slot_count, LANES)
    total = jnp.zeros((tokens, LANES), F32)
    for k in (0, 1):
        pick = (where_at == slot_ref[:, k : k + 1]).astype(F32).astype(BF16)
        total = total + dot(pick, rets) * rw_ref[:, k : k + 1]
    expert_ref[...] = total.astype(BF16)

    for d in pending:
        d.wait_send()


def rotary_tables(tokens):
    half_width = ROPE // 2
    positions = (lax.axis_index("ep") * tokens + jnp.arange(tokens, dtype=jnp.int32)).astype(F32)
    frequencies = ROTARY_BASE ** (-jnp.arange(half_width, dtype=F32) / half_width)
    angles = positions[:, None] * frequencies[None, :]
    return jnp.cos(angles), jnp.sin(angles)


def local(
    dims,
    query_latent, joint_latent, rotary_key, query_gain, joint_gain, query_weight, query_rotary,
    key_weight, value_weight, output_weight, expert_input, expert_gain, routes, route_weight,
    gate_weight, up_weight, down_weight,
):
    ny, nx, nz = dims
    ep_n, tokens, width = ny * nx, query_latent.shape[0], output_weight.shape[1]
    cap = 3 * tokens // (2 * ep_n)
    experts = 2 * ep_n
    rows = ep_n * cap
    half = tokens // 2
    hw = ROPE // 2

    cos, sin = rotary_tables(tokens)
    k1, k2 = rotary_key[:, :hw].astype(F32), rotary_key[:, hw:].astype(F32)
    turned_t = jnp.concatenate([k1 * cos - k2 * sin, k2 * cos + k1 * sin], axis=1).astype(BF16).T

    def placed(plain0, rope0, rope1, plain1, n):
        pad = jnp.zeros((n, ROPE), plain0.dtype)
        return jnp.concatenate([plain0, rope0, pad, pad, rope1, plain1], axis=1)

    def swapped(w):
        return jnp.concatenate([w[:, hw:], w[:, :hw]], axis=1)

    depth = query_weight.shape[0]
    none = jnp.zeros((depth, NOPE), BF16)
    wa = placed(query_weight[:, :NOPE], query_rotary[:, :ROPE], query_rotary[:, ROPE:], query_weight[:, NOPE:], depth)
    wb = placed(none, swapped(query_rotary[:, :ROPE]), swapped(query_rotary[:, ROPE:]), none, depth)
    cc = jnp.concatenate([cos, cos], axis=1)
    ss = jnp.concatenate([-sin, sin], axis=1)
    one = jnp.ones((tokens, NOPE), F32)
    cq = placed(one, cc, cc, one, tokens)
    sq = placed(one * 0, ss, ss, one * 0, tokens)

    sds = jax.ShapeDtypeStruct
    slots, kt_own, v_own, q, slot = pl.pallas_call(
        functools.partial(front_kernel, cap, experts),
        out_shape=(
            sds((experts, cap, LANES), BF16),
            sds((2, LANES + ROPE, half), BF16),
            sds((2, half, LANES), BF16),
            sds((tokens, 2 * LANES), BF16),
            sds((tokens, 2), jnp.int32),
        ),
        compiler_params=pltpu.CompilerParams(vmem_limit_bytes=56 * 2**20),
        name="front",
    )(
        query_latent, joint_latent, turned_t, query_gain[None], joint_gain[None], wa, wb, cq, sq,
        key_weight.T, value_weight, expert_input, expert_gain[None], routes, routes.T,
    )
    slots = slots.reshape(ep_n, 2, cap, LANES)

    hz = nz // 2
    per = tokens // (2 * nz)
    vmem = pl.BlockSpec(memory_space=pltpu.VMEM)
    hbm = pl.BlockSpec(memory_space=pl.ANY)
    sem = pltpu.SemaphoreType.DMA
    scratch = [
        pltpu.VMEM((2, nz, 2, rows, LANES), BF16),
        pltpu.VMEM((2, nz, 2, rows, LANES), BF16),
        pltpu.VMEM((2, nz, rows, LANES), BF16),
        pltpu.VMEM((2, 2, hz, rows, LANES), BF16),
        pltpu.VMEM((2, 2, hz, rows, LANES), BF16),
        pltpu.VMEM((2, rows, LANES), BF16),
        pltpu.VMEM((experts, cap, LANES), BF16),
        pltpu.VMEM((2, max(ny, nx), max(ny, nx), LANES + ROPE, half), BF16),
        pltpu.VMEM((2, max(ny, nx), max(ny, nx), half, LANES), BF16),
        pltpu.VMEM(gate_weight.shape, BF16),
        pltpu.VMEM(up_weight.shape, BF16),
        pltpu.VMEM(down_weight.shape, BF16),
        pltpu.VMEM((2, tokens, LANES), F32),
        pltpu.VMEM((2, tokens, LANES), F32),
        pltpu.VMEM((2, tokens, LANES), F32),
        pltpu.VMEM((nz, 2, per, width), BF16),
        pltpu.VMEM((nz, per, width), BF16),
        pltpu.VMEM((2, hz, per, width), BF16),
        pltpu.VMEM((2, hz, per, width), BF16),
        sem((ep_n,)), sem((ep_n,)),
        sem((2, 2, hz)), sem((2, 2, hz)),
        sem((2, 2, hz + 1)), sem((2, 2, hz + 1)),
        sem((2, 2, 2, 2, 2)), sem((2, 2, 2, 2, 2)),
        sem((2,)), sem((2,)),
        sem((2, 2, hz)), sem((2, 2, hz)),
        sem((2, ep_n)), sem((2, ep_n)),
        sem(()), sem(()),
        sem((2, hz)), sem((2, hz)),
        sem((8,)),
    ]
    mixer, expert = pl.pallas_call(
        functools.partial(main_kernel, (ny, nx, nz, cap)),
        out_shape=(sds((per, width), BF16), sds((tokens, LANES), BF16)),
        in_specs=[vmem, hbm, hbm, vmem, vmem, vmem, hbm, hbm, hbm, vmem],
        out_specs=(vmem, vmem),
        scratch_shapes=scratch,
        compiler_params=pltpu.CompilerParams(
            collective_id=0, has_side_effects=True, vmem_limit_bytes=62 * 2**20
        ),
        name="main",
    )(slots, kt_own, v_own, q, slot, route_weight, gate_weight, up_weight, down_weight, output_weight)
    return mixer, expert


def solution(mesh):
    ny, nx = ep_grid(mesh.shape["ep"])
    return jax.shard_map(
        functools.partial(local, (ny, nx, mesh.shape["tp"] // 2)),
        mesh=mesh,
        in_specs=(
            P("ep", None),
            P("ep", None),
            P("ep", None),
            P(),
            P(),
            P(None, "tp"),
            P(None, "tp"),
            P(None, "tp"),
            P(None, "tp"),
            P("tp", None),
            P("ep", None),
            P(),
            P("ep", None),
            P("ep", None),
            P("ep", None, "tp"),
            P("ep", None, "tp"),
            P("ep", "tp", None),
        ),
        out_specs=(P(("ep", "tp"), None), P("ep", "tp")),
        check_vma=False,
    )
```

```python
import functools

import jax
import jax.numpy as jnp
from jax import lax
from jax.experimental import pallas as pl
from jax.experimental.pallas import tpu as pltpu
from jax.sharding import PartitionSpec as P

NOPE = 64
VDIM = 64
ROPE = 32
NORM_EPSILON = 1e-06
ROTARY_BASE = 10000.0
LANES = 128
LOG2E = 1.4426950408889634
MESH = pl.DeviceIdType.MESH
F32 = jnp.float32
BF16 = jnp.bfloat16


def ep_grid(count):
    return {16: (4, 4), 4: (2, 2), 2: (1, 2)}[count]


def dot(a, b):
    return jnp.dot(a, b, preferred_element_type=F32)


def dot_nt(a, b):
    return lax.dot_general(a, b, (((1,), (1,)), ((), ())), preferred_element_type=F32)


def main_kernel(
    dims,
    routes_ref, rw_ref, qgain, jgain, egain, rk_ref, cos_ref, sin_ref,
    xin_hbm, jl_hbm, wk_hbm, wv_hbm, ql_hbm, wq_hbm, wr_hbm, wg_hbm, wu_hbm, wd_hbm, wo_hbm,
    mixer_ref, expert_ref,
    xin, jl, wk, wv, ql, wq, wr, wg, wu, wd, wo,
    slots, xbuf, pbuf, sbuf, rbuf, tbuf, fin, ret, ktb, vb, q_s, cols, m_s, l_s, acc_s,
    ap, asb, arb, atb,
    a2a_s, a2a_r, zs, zr, dds, ddr, kvs, kvr, pss, psr, rss, rsr, bks, bkr, aps, apr, ars, arr, local_s, own_s,
):
    ny, nx, nz, cap = dims
    ep_n = ny * nx
    experts = 2 * ep_n
    rows = ep_n * cap
    ns = nz // 2
    ep = lax.axis_index("ep")
    tp = lax.axis_index("tp")
    y, x = ep // nx, lax.rem(ep, nx)
    z, c = tp // 2, lax.rem(tp, 2)
    par = lax.rem(z, 2)
    opar = 1 - par
    oc = 1 - c
    zright = lax.rem(z + 1, nz)
    zleft = lax.rem(z + nz - 1, nz)
    z_to = ((ep, zright * 2 + c), (ep, zleft * 2 + c))
    sib = (ep, z * 2 + oc)
    tokens = xin.shape[0]
    half = tokens // 2
    pending = []

    def send(src, dst, ssem, rsem, to):
        d = pltpu.make_async_remote_copy(
            src_ref=src, dst_ref=dst, send_sem=ssem, recv_sem=rsem, device_id=to, device_id_type=MESH
        )
        d.start()
        pending.append(d)

    def arrived(dst, ssem, rsem, frm):
        pltpu.make_async_remote_copy(
            src_ref=dst, dst_ref=dst, send_sem=ssem, recv_sem=rsem, device_id=frm, device_id_type=MESH
        ).wait_recv()

    barrier = pltpu.get_barrier_semaphore()
    peers = [(lax.rem(ep + k, ep_n), tp) for k in range(1, ep_n)]
    peers.append(sib)
    peers.append(z_to[0])
    if nz > 2:
        peers.append(z_to[1])
    for peer in peers:
        pl.semaphore_signal(barrier, inc=1, device_id=peer, device_id_type=MESH)

    loads = {}
    for i, (name, src, dst) in enumerate(
        (
            ("xin", xin_hbm, xin), ("jl", jl_hbm, jl), ("wk", wk_hbm, wk), ("wv", wv_hbm, wv),
            ("ql", ql_hbm, ql), ("wq", wq_hbm, wq), ("wr", wr_hbm, wr), ("wg", wg_hbm, wg),
            ("wu", wu_hbm, wu), ("wd", wd_hbm, wd), ("wo", wo_hbm, wo),
        )
    ):
        loads[name] = pltpu.make_async_copy(src, dst, local_s.at[i])
        loads[name].start()

    with jax.named_scope("routing"):
        row = lax.broadcasted_iota(jnp.int32, (tokens, tokens), 0)
        col = lax.broadcasted_iota(jnp.int32, (tokens, tokens), 1)
        sub_e = lax.broadcasted_iota(jnp.int32, (experts, tokens), 0)
        named0 = sub_e == routes_ref[0:1, :]
        named1 = sub_e == routes_ref[1:2, :]
        named = named0 | named1
        before = dot(named.astype(F32).astype(BF16), (row < col).astype(F32).astype(BF16))
        rank = jnp.where(named, before, -1.0)
        place = before + (sub_e * cap).astype(F32)
        slot0 = jnp.sum(jnp.where(named0, place, 0.0), axis=0, keepdims=True)
        slot1 = jnp.sum(jnp.where(named1, place, 0.0), axis=0, keepdims=True)
        stack = jnp.concatenate([slot0, slot1, rw_ref[...], jnp.zeros((4, tokens), F32)], axis=0)
        cols[...] = stack.T

    with jax.named_scope("expert_norm"):
        loads["xin"].wait()
        xf = xin[...].astype(F32)
        factor = lax.rsqrt(jnp.mean(xf * xf, axis=-1, keepdims=True) + NORM_EPSILON)
        mine = []
        for i in range(ns):
            at = pl.ds(pl.multiple_of((4 * i + 2 * par + c) * LANES, LANES), LANES)
            mine.append((xin[:, at].astype(F32) * factor * egain[:, at]).astype(BF16))
        mine = jnp.concatenate(mine, axis=1)
        place_in = lax.broadcasted_iota(jnp.int32, (cap, tokens), 0).astype(F32)

    groups = [pl.ds(0, ns)] if ns == 1 else [pl.ds(0, ns // 2), pl.ds(ns // 2, ns - ns // 2)]
    members = [range(g.start, g.start + g.size) for g in groups]
    mine_rows = pl.ds(pl.multiple_of(ep * cap, 16), cap)

    def dispatch(e):
        group = min(8, ep_n)
        with jax.named_scope("slots"):
            for d0 in range(0, ep_n, group):
                pick = [
                    (place_in == rank[2 * d + e : 2 * d + e + 1, :]).astype(F32).astype(BF16)
                    for d in range(d0, d0 + group)
                ]
                out = dot(jnp.concatenate(pick, axis=0), mine).astype(BF16)
                for d in range(group):
                    for i in range(ns):
                        slots[e, d0 + d, i] = out[d * cap : (d + 1) * cap, i * LANES : (i + 1) * LANES]
        if e == 0:
            with jax.named_scope("barrier"):
                pl.semaphore_wait(barrier, len(peers))
        for g, span in enumerate(groups):
            for k in range(1, ep_n):
                to = lax.rem(ep + k, ep_n)
                there = xbuf.at[e, span, par, c, mine_rows]
                send(slots.at[e, to, span], there, a2a_s.at[e, g, k], a2a_r.at[e, g, k], (to, tp))
        pltpu.make_async_copy(slots.at[e, ep], xbuf.at[e, :, par, c, mine_rows], own_s.at[e]).start()

    axes = (("x", nx, x), ("y", ny, y))

    def ring_to(name, step):
        if name == "x":
            return (y * nx + lax.rem(x + nx + step, nx), tp)
        return (lax.rem(y + ny + step, ny) * nx + x, tp)

    def kv_refs(part, phase, block, j):
        other = (y, x)[part]
        if phase == 0:
            return ktb.at[part, other, block], vb.at[part, other, block]
        n, me = ((nx, x), (ny, y))[part]
        b = lax.rem(me + j, n)
        return ktb.at[part, block, b], vb.at[part, block, b]

    def kv_copies(part, phase, step, j, arriving):
        name, n, me = axes[(part + phase) % 2]
        if n == 1 or step > n // 2:
            return
        tie = 2 * step == n
        for d, sign in ((0, 1), (1, -1)):
            block = lax.rem(me + n - sign * (step if arriving else step - 1), n)
            refs = kv_refs(part, phase, block, j)
            for kind in (0, 1):
                if not tie or kind == d:
                    i = (part, phase * 4 + j, d, step - 1, kind)
                    if arriving:
                        arrived(refs[kind], kvs.at[i], kvr.at[i], ring_to(name, -sign))
                    else:
                        send(refs[kind], refs[kind], kvs.at[i], kvr.at[i], ring_to(name, sign))

    def kv_js(part, step):
        n = (nx, ny)[part]
        return ([0], sorted({1, n - 1} - {0, n}), [2] if n == 4 else [])[step]

    def kv_line(step):
        with jax.named_scope(f"kv_line#s={step}"):
            for part in (0, 1):
                if step:
                    kv_copies(part, 0, step, 0, True)
                kv_copies(part, 0, step + 1, 0, False)
                for j in kv_js(part, step):
                    kv_copies(part, 1, 1, j, False)

    def kv_plane(step, pieces):
        with jax.named_scope(f"kv_plane#s={step}"):
            for part in (0, 1):
                for piece in pieces:
                    for j in kv_js(part, piece):
                        kv_copies(part, 1, step, j, True)
                        kv_copies(part, 1, step + 1, j, False)

    def normed(ref, gain):
        v = ref[...].astype(F32)
        f = lax.rsqrt(jnp.mean(v * v, axis=-1, keepdims=True) + NORM_EPSILON)
        return (v * f * gain[...]).astype(BF16)

    lane = lax.broadcasted_iota(jnp.int32, (tokens, LANES), 1)
    scale = LOG2E * (NOPE + ROPE) ** (-0.5)

    def turned(u):
        left = pltpu.roll(u, LANES - ROPE // 2, 1)
        right = pltpu.roll(u, ROPE // 2, 1)
        other = jnp.where(lax.rem(lane, ROPE) < ROPE // 2, left, right)
        return u * cos_ref[...] + other * sin_ref[...]

    def keys_values():
        with jax.named_scope("kv_proj"):
            for name in ("jl", "wk", "wv"):
                loads[name].wait()
            jn = normed(jl, jgain)
            kt = dot(jn, wk[...]).T.astype(BF16)
            wide = jnp.concatenate([rk_ref[...].astype(F32), jnp.zeros((LANES - ROPE, tokens), F32)], axis=0)
            rt = turned(wide.T).T[0:ROPE].astype(BF16)
            vv = dot(jn, wv[...]).astype(BF16)
            for h, (a, b) in enumerate(((y, x), (x, y))):
                part = slice(h * half, (h + 1) * half)
                ktb[h, a, b, 0:NOPE, :] = kt[0:NOPE, part]
                ktb[h, a, b, NOPE : NOPE + ROPE, :] = rt[:, part]
                ktb[h, a, b, NOPE + ROPE :, :] = kt[NOPE:, part]
                vb[h, a, b] = vv[part]
        kv_line(0)

    def queries():
        with jax.named_scope("q_proj"):
            for name in ("ql", "wq", "wr"):
                loads[name].wait()
            qn = normed(ql, qgain)
            plain = dot(qn, wq[...])
            rope = dot_nt(qn, wr[...])
            rope = turned(jnp.concatenate([rope, jnp.zeros((tokens, LANES - 2 * ROPE), F32)], axis=1))
            first = jnp.where(lane < NOPE, plain, jnp.where(lane < NOPE + ROPE, pltpu.roll(rope, NOPE, 1), 0.0))
            second = jnp.where(lane < ROPE, 0.0, jnp.where(lane < NOPE, rope, plain))
            q_s[0] = (first * scale).astype(BF16)
            q_s[1] = (second * scale).astype(BF16)

    def a2a_wait(e, g):
        if g >= len(groups):
            return
        span = groups[g]
        with jax.named_scope(f"a2a_wait#e={e}#g={g}"):
            if g == 0:
                pltpu.make_async_copy(slots.at[e, ep], xbuf.at[e, :, par, c, mine_rows], own_s.at[e]).wait()
            for k in range(1, ep_n):
                frm = lax.rem(ep + ep_n - k, ep_n)
                there = xbuf.at[e, span, par, c, pl.ds(pl.multiple_of(frm * cap, 16), cap)]
                arrived(there, a2a_s.at[e, g, k], a2a_r.at[e, g, k], (frm, tp))
        for i in members[g]:
            piece = xbuf.at[e, i, par, c]
            send(piece, piece, zs.at[e, i], zr.at[e, i], z_to[i % 2])
        piece = xbuf.at[e, span, par, c]
        send(piece, piece, dds.at[e, ns + g], ddr.at[e, ns + g], sib)

    def z_wait(e, g):
        if g >= len(groups):
            return
        with jax.named_scope(f"z_wait#e={e}#g={g}"):
            for i in members[g]:
                piece = xbuf.at[e, i, opar, c]
                arrived(piece, zs.at[e, i], zr.at[e, i], z_to[1 - i % 2])
                send(piece, piece, dds.at[e, i], ddr.at[e, i], sib)

    row_tile = 256 if rows % 256 == 0 else rows // 2

    def pair_copy(e, t):
        at = pl.ds(pl.multiple_of(t * row_tile, row_tile), row_tile)
        return pltpu.make_async_remote_copy(
            src_ref=pbuf.at[e, :, oc, at], dst_ref=sbuf.at[e, :, at], send_sem=pss.at[e, t], recv_sem=psr.at[e, t],
            device_id=sib, device_id_type=MESH,
        )

    def expert(e):
        with jax.named_scope(f"dd_wait#e={e}"):
            for g, span in enumerate(groups):
                arrived(xbuf.at[e, span, par, oc], dds.at[e, ns + g], ddr.at[e, ns + g], sib)
            for i in range(ns):
                arrived(xbuf.at[e, i, opar, oc], dds.at[e, i], ddr.at[e, i], sib)

        def tile(t, carry):
            at = pl.ds(pl.multiple_of(t * row_tile, row_tile), row_tile)
            xx = jnp.concatenate([xbuf[e, j // 4, j // 2 % 2, j % 2, at] for j in range(2 * nz)], axis=1)
            gate = dot(xx, wg[e])
            up = dot(xx, wu[e])
            hidden = (gate / (1.0 + jnp.exp(-gate)) * up).astype(BF16)
            part = dot(hidden, wd[e]).astype(BF16)
            for j in range(2 * nz):
                pbuf[e, j // 2, j % 2, at] = part[:, j * LANES : (j + 1) * LANES]
            pair_copy(e, t).start()
            return carry

        with jax.named_scope(f"expert#e={e}"):
            lax.fori_loop(0, rows // row_tile, tile, 0)
        for t in range(rows // row_tile):
            pending.append(pair_copy(e, t))

    hz = nz // 2

    def reducer(name, p, s, r, t, ssem, rsem):
        cut = p.shape[2] // 2

        def term(dest, at):
            return p[dest, c, at].astype(F32) + s[dest, at].astype(F32)

        def put(own, step):
            if step > hz:
                return
            for d, sign in ((0, 1), (1, -1)):
                g = d if own else 1 - d
                at = pl.ds(g * cut, cut)
                dest = lax.rem(z + sign * (hz + 1 - step) + nz, nz)
                v = term(dest, at)
                if step > (1 if own else 2):
                    v = v + r[d, step - 2, at].astype(F32)
                t[d, step - 1, at] = v.astype(BF16)
                i = (d, g, step - 1)
                send(t.at[d, step - 1, at], r.at[d, step - 1, at], ssem.at[i], rsem.at[i], z_to[d])

        def take(own, step):
            for d in (0, 1):
                g = d if own else 1 - d
                at = pl.ds(g * cut, cut)
                i = (d, g, step - 1)
                arrived(r.at[d, step - 1, at], ssem.at[i], rsem.at[i], z_to[1 - d])

        events = []
        for step in range(1, hz + 1):
            events.append((True, step))
            if step < hz:
                events.append((False, step + 1))

        def start():
            with jax.named_scope(f"start#{name}"):
                put(True, 1)
                put(False, 2)

        def event():
            own, step = events.pop(0)
            with jax.named_scope(f"take#{name}#own={int(own)}#s={step}"):
                take(own, step)
            put(own, step + 1)

        def last():
            out = []
            for g in (0, 1):
                at = pl.ds(g * cut, cut)
                v = term(z, at)
                for d in (0, 1):
                    if hz > 1 or g == d:
                        v = v + r[d, hz - 1, at].astype(F32)
                out.append(v.astype(BF16))
            return out

        return start, event, last, events

    hr = rows // 2

    def finish(e, last):
        with jax.named_scope(f"finish#e={e}"):
            for g, v in enumerate(last()):
                fin[e, g * hr : (g + 1) * hr] = v
            for k in range(1, ep_n):
                to = lax.rem(ep + k, ep_n)
                src = fin.at[e, pl.ds(pl.multiple_of(to * cap, 16), cap)]
                send(src, ret.at[2 * ep + e], bks.at[e, k], bkr.at[e, k], (to, tp))
            ret[2 * ep + e] = fin[e, mine_rows]

    q_tile = min(256, tokens)

    def unit(part, a):
        blocks = (nx, ny)[part]

        def tile(t):
            at = pl.ds(t * q_tile, q_tile)
            both = []
            for head in (0, 1):
                q = q_s[head, at]
                both.append([dot(q, ktb[part, a, b, head * ROPE : head * ROPE + LANES, :]) for b in range(blocks)])
            vals = jnp.concatenate([vb[part, a, b] for b in range(blocks)], axis=0)
            for head, s in enumerate(both):
                m_old = m_s[head, at]
                m_new = jnp.maximum(m_old, jnp.max(functools.reduce(jnp.maximum, s), axis=1, keepdims=True))
                alpha = jnp.exp2(m_old - m_new)
                m_s[head, at] = m_new
                p = [jnp.exp2(v[:, i : i + LANES] - m_new) for v in s for i in range(0, half, LANES)]
                l_s[head, at] = l_s[head, at] * alpha + functools.reduce(jnp.add, p)
                p = jnp.concatenate([v.astype(BF16) for v in p], axis=1)
                acc_s[head, at] = acc_s[head, at] * alpha + dot(p, vals)

        return tile

    a0 = (y, x)
    alen = (ny, nx)
    tiles = tokens // q_tile
    todo = []
    for near in ((0,), (1, 2), (3,)):
        pairs = [(part, i) for i in near for part in (0, 1) if i < alen[part]]
        if near == (3,) or max(alen) < 4:
            todo += [(part, i, t) for t in range(tiles) for part, i in pairs]
        else:
            todo += [(part, i, t) for part, i in pairs for t in range(tiles)]

    def some(count=1):
        for _ in range(count):
            if todo:
                part, i, t = todo.pop(0)
                off = (0, alen[part] - 1, 1, 2)[i] if alen[part] > 2 else i
                with jax.named_scope(f"unit#n={len(todo)}"):
                    unit(part, lax.rem(a0[part] + off, alen[part]))(t)

    red = [
        reducer(f"e{e}", pbuf.at[e], sbuf.at[e], rbuf.at[e], tbuf.at[e], rss.at[e], rsr.at[e]) for e in (0, 1)
    ]

    def pair(e):
        with jax.named_scope(f"pair#e={e}"):
            for t in range(rows // row_tile):
                pair_copy(e, t).wait_recv()

    def out_proj():
        with jax.named_scope("out_proj"):
            loads["wo"].wait()
            t0 = jnp.sum(l_s[0], axis=1, keepdims=True)
            t1 = jnp.sum(l_s[1], axis=1, keepdims=True)
            attended = jnp.where(lane < VDIM, acc_s[0] / t0, acc_s[1] / t1).astype(BF16)
            per = tokens // (2 * nz)
            for q in range(0, nz, hz):
                proj = dot(attended[q * 2 * per : (q + hz) * 2 * per], wo[...]).astype(BF16)
                for i in range(2 * hz):
                    ap[q + i // 2, i % 2] = proj[i * per : (i + 1) * per]
                span = pl.ds(q, hz)
                send(ap.at[span, oc], asb.at[span], aps.at[q // hz], apr.at[q // hz], sib)

    def combine():
        with jax.named_scope("combine_wait"):
            for e in (0, 1):
                for k in range(1, ep_n):
                    frm = lax.rem(ep + ep_n - k, ep_n)
                    arrived(ret.at[2 * frm + e], bks.at[e, k], bkr.at[e, k], (frm, tp))
        with jax.named_scope("combine"):
            slot_count = experts * cap
            where_at = lax.broadcasted_iota(jnp.int32, (tokens, slot_count), 1).astype(F32)
            rets = ret[...].reshape(slot_count, LANES)
            total = jnp.zeros((tokens, LANES), F32)
            for k in (0, 1):
                pick = (where_at == cols[:, k : k + 1]).astype(F32).astype(BF16)
                total = total + dot(pick, rets) * cols[:, 2 + k : 3 + k]
            expert_ref[...] = total.astype(BF16)

    red.append(reducer("a", ap, asb, arb, atb, ars, arr))

    def step_of(e):
        if red[e][3]:
            red[e][1]()
            if e < 2 and not red[e][3]:
                finish(e, red[e][2])

    kv_state = []

    def kv_upto(count):
        for stage in range(len(kv_state) + 1, count + 1):
            kv_state.append(stage)
            if stage == 1:
                kv_plane(1, (0, 1))
            elif stage == 2:
                kv_plane(1, (2,))
            else:
                kv_plane(2, (0, 1, 2))

    def work(count):
        for _ in range(count):
            if not todo:
                return
            if len(todo) <= 6 * tiles:
                kv_upto(2)
            if len(todo) <= 2 * tiles:
                kv_upto(3)
            some()

    dispatch(0)
    dispatch(1)
    keys_values()
    m_s[...] = jnp.full(m_s.shape, -jnp.inf, F32)
    l_s[...] = jnp.zeros(l_s.shape, F32)
    acc_s[...] = jnp.zeros(acc_s.shape, F32)
    queries()
    a2a_wait(0, 0)
    a2a_wait(0, 1)
    a2a_wait(1, 0)
    z_wait(0, 0)
    a2a_wait(1, 1)
    z_wait(0, 1)
    for name in ("wg", "wu", "wd"):
        loads[name].wait()
    expert(0)
    kv_line(1)
    z_wait(1, 0)
    pair(0)
    red[0][0]()
    z_wait(1, 1)
    expert(1)
    step_of(0)
    pair(1)
    red[1][0]()
    step_of(0)
    kv_line(2)
    work(1)
    step_of(0)
    work(1)
    step_of(0)
    work(2)
    step_of(1)
    kv_upto(1)
    step_of(1)
    step_of(0)
    kv_upto(2)
    work(2)
    for e in (0, 1, 1, 0):
        step_of(e)
        work(2)
    step_of(1)
    kv_upto(3)
    work(len(todo))
    out_proj()
    step_of(0)
    with jax.named_scope("pair#a"):
        for q in range(0, nz, hz):
            arrived(asb.at[pl.ds(q, hz)], aps.at[q // hz], apr.at[q // hz], sib)
    red[2][0]()
    for e in (1, 2, 1, 2, 1, 2, 2):
        step_of(e)
    for e in (0, 1):
        while red[e][3]:
            step_of(e)
    while len(red[2][3]) > 1:
        step_of(2)
    combine()
    while red[2][3]:
        step_of(2)
    cut = mixer_ref.shape[0] // 2
    for g, v in enumerate(red[2][2]()):
        mixer_ref[g * cut : (g + 1) * cut] = v

    for d in pending:
        d.wait_send()


def back_kernel(mixer, expert, mixer_out, expert_out):
    mixer_out[...] = mixer[...]
    expert_out[...] = expert[...]


def rotary_tables(tokens):
    half_width = ROPE // 2
    positions = (lax.axis_index("ep") * tokens + jnp.arange(tokens, dtype=jnp.int32)).astype(F32)
    lanes = jnp.arange(LANES, dtype=jnp.int32) % ROPE
    frequencies = ROTARY_BASE ** (-(lanes % half_width).astype(F32) / half_width)
    angles = positions[:, None] * frequencies[None, :]
    sine = jnp.sin(angles)
    return jnp.cos(angles), jnp.where(lanes[None, :] < half_width, -sine, sine)


def local(
    dims,
    query_latent, joint_latent, rotary_key, query_gain, joint_gain, query_weight, query_rotary,
    key_weight, value_weight, output_weight, expert_input, expert_gain, routes, route_weight,
    gate_weight, up_weight, down_weight,
):
    ny, nx, nz = dims
    ep_n, tokens, width = ny * nx, query_latent.shape[0], output_weight.shape[1]
    cap = 3 * tokens // (2 * ep_n)
    rows = ep_n * cap
    half = tokens // 2
    cos, sin = rotary_tables(tokens)

    hz = nz // 2
    per = tokens // (2 * nz)
    sds = jax.ShapeDtypeStruct
    vmem = pl.BlockSpec(memory_space=pltpu.VMEM)
    hbm = pl.BlockSpec(memory_space=pl.ANY)
    sem = pltpu.SemaphoreType.DMA
    side = max(ny, nx)
    streamed = [
        expert_input, joint_latent, key_weight, value_weight, query_latent, query_weight, query_rotary.T,
        gate_weight, up_weight, down_weight, output_weight,
    ]
    scratch = [pltpu.VMEM(a.shape, a.dtype) for a in streamed] + [
        pltpu.VMEM((2, ep_n, hz, cap, LANES), BF16),
        pltpu.VMEM((2, hz, 2, 2, rows, LANES), BF16),
        pltpu.VMEM((2, nz, 2, rows, LANES), BF16),
        pltpu.VMEM((2, nz, rows, LANES), BF16),
        pltpu.VMEM((2, 2, hz, rows, LANES), BF16),
        pltpu.VMEM((2, 2, hz, rows, LANES), BF16),
        pltpu.VMEM((2, rows, LANES), BF16),
        pltpu.VMEM((2 * ep_n, cap, LANES), BF16),
        pltpu.VMEM((2, side, side, LANES + ROPE, half), BF16),
        pltpu.VMEM((2, side, side, half, LANES), BF16),
        pltpu.VMEM((2, tokens, LANES), BF16),
        pltpu.VMEM((tokens, 8), F32),
        pltpu.VMEM((2, tokens, LANES), F32),
        pltpu.VMEM((2, tokens, LANES), F32),
        pltpu.VMEM((2, tokens, LANES), F32),
        pltpu.VMEM((nz, 2, per, width), BF16),
        pltpu.VMEM((nz, per, width), BF16),
        pltpu.VMEM((2, hz, per, width), BF16),
        pltpu.VMEM((2, hz, per, width), BF16),
        sem((2, 2, ep_n)), sem((2, 2, ep_n)),
        sem((2, hz)), sem((2, hz)),
        sem((2, hz + 2)), sem((2, hz + 2)),
        sem((2, 8, 2, 2, 2)), sem((2, 8, 2, 2, 2)),
        sem((2, 4)), sem((2, 4)),
        sem((2, 2, 2, hz)), sem((2, 2, 2, hz)),
        sem((2, ep_n)), sem((2, ep_n)),
        sem((2,)), sem((2,)),
        sem((2, 2, hz)), sem((2, 2, hz)),
        sem((len(streamed),)),
        sem((2,)),
    ]
    mixer, expert = pl.pallas_call(
        functools.partial(main_kernel, (ny, nx, nz, cap)),
        out_shape=(sds((per, width), BF16), sds((tokens, LANES), BF16)),
        in_specs=[vmem] * 8 + [hbm] * len(streamed),
        out_specs=(vmem, vmem),
        scratch_shapes=scratch,
        compiler_params=pltpu.CompilerParams(
            collective_id=0, has_side_effects=True, vmem_limit_bytes=62 * 2**20
        ),
        name="main",
    )(
        routes.T, route_weight.T, query_gain[None], joint_gain[None], expert_gain[None], rotary_key.T, cos, sin,
        *streamed,
    )
    return pl.pallas_call(
        back_kernel,
        out_shape=(sds(mixer.shape, BF16), sds(expert.shape, BF16)),
        name="back",
    )(mixer, expert)


def solution(mesh):
    ny, nx = ep_grid(mesh.shape["ep"])
    return jax.shard_map(
        functools.partial(local, (ny, nx, mesh.shape["tp"] // 2)),
        mesh=mesh,
        in_specs=(
            P("ep", None),
            P("ep", None),
            P("ep", None),
            P(),
            P(),
            P(None, "tp"),
            P(None, "tp"),
            P(None, "tp"),
            P(None, "tp"),
            P("tp", None),
            P("ep", None),
            P(),
            P("ep", None),
            P("ep", None),
            P("ep", None, "tp"),
            P("ep", None, "tp"),
            P("ep", "tp", None),
        ),
        out_specs=(P(("ep", "tp"), None), P("ep", "tp")),
        check_vma=False,
    )
```

```python
import functools

import jax
import jax.numpy as jnp
from jax import lax
from jax.experimental import pallas as pl
from jax.experimental.pallas import tpu as pltpu
from jax.sharding import PartitionSpec as P

NOPE = 64
VDIM = 64
ROPE = 32
NORM_EPSILON = 1e-06
ROTARY_BASE = 10000.0
LANES = 128
LOG2E = 1.4426950408889634
MESH = pl.DeviceIdType.MESH
F32 = jnp.float32
BF16 = jnp.bfloat16


def ep_grid(count):
    return {16: (4, 4), 4: (2, 2), 2: (1, 2)}[count]


def dot(a, b):
    return jnp.dot(a, b, preferred_element_type=F32)


def dot_nt(a, b):
    return lax.dot_general(a, b, (((1,), (1,)), ((), ())), preferred_element_type=F32)


def main_kernel(
    dims,
    routes_ref, rw_ref, qgain, jgain, egain, rk_ref, cos_ref, sin_ref,
    xin_hbm, jl_hbm, wk_hbm, wv_hbm, ql_hbm, wq_hbm, wr_hbm, wg_hbm, wu_hbm, wd_hbm, wo_hbm,
    mixer_ref, expert_ref,
    xin, jl, wk, wv, ql, wq, wr, wg, wu, wd, wo,
    slots, xbuf, pbuf, sbuf, rbuf, tbuf, fin, ret, ktb, vb, q_s, cols, m_s, l_s, acc_s,
    ap, asb, arb, atb,
    a2a_s, a2a_r, zs, zr, dds, ddr, kvs, kvr, pss, psr, rss, rsr, bks, bkr, aps, apr, ars, arr, local_s, own_s,
):
    ny, nx, nz, cap = dims
    ep_n = ny * nx
    experts = 2 * ep_n
    rows = ep_n * cap
    ns = nz // 2
    ep = lax.axis_index("ep")
    tp = lax.axis_index("tp")
    y, x = ep // nx, lax.rem(ep, nx)
    z, c = tp // 2, lax.rem(tp, 2)
    par = lax.rem(z, 2)
    opar = 1 - par
    oc = 1 - c
    zright = lax.rem(z + 1, nz)
    zleft = lax.rem(z + nz - 1, nz)
    z_to = ((ep, zright * 2 + c), (ep, zleft * 2 + c))
    sib = (ep, z * 2 + oc)
    tokens = xin.shape[0]
    half = tokens // 2
    pending = []

    def send(src, dst, ssem, rsem, to):
        d = pltpu.make_async_remote_copy(
            src_ref=src, dst_ref=dst, send_sem=ssem, recv_sem=rsem, device_id=to, device_id_type=MESH
        )
        d.start()
        pending.append(d)

    def flush(count):
        with jax.named_scope(f"flush#n={count}"):
            for _ in range(min(count, len(pending))):
                pending.pop(0).wait_send()

    def arrived(dst, ssem, rsem, frm):
        pltpu.make_async_remote_copy(
            src_ref=dst, dst_ref=dst, send_sem=ssem, recv_sem=rsem, device_id=frm, device_id_type=MESH
        ).wait_recv()

    barrier = pltpu.get_barrier_semaphore()
    peers = [(lax.rem(ep + k, ep_n), tp) for k in range(1, ep_n)]
    peers.append(sib)
    peers.append(z_to[0])
    if nz > 2:
        peers.append(z_to[1])
    for peer in peers:
        pl.semaphore_signal(barrier, inc=1, device_id=peer, device_id_type=MESH)

    loads = {}
    for i, (name, src, dst) in enumerate(
        (
            ("xin", xin_hbm, xin), ("jl", jl_hbm, jl), ("wk", wk_hbm, wk), ("wv", wv_hbm, wv),
            ("ql", ql_hbm, ql), ("wq", wq_hbm, wq), ("wr", wr_hbm, wr), ("wg", wg_hbm, wg),
            ("wu", wu_hbm, wu), ("wd", wd_hbm, wd), ("wo", wo_hbm, wo),
        )
    ):
        loads[name] = pltpu.make_async_copy(src, dst, local_s.at[i])
        loads[name].start()

    with jax.named_scope("routing"):
        row = lax.broadcasted_iota(jnp.int32, (tokens, tokens), 0)
        col = lax.broadcasted_iota(jnp.int32, (tokens, tokens), 1)
        sub_e = lax.broadcasted_iota(jnp.int32, (experts, tokens), 0)
        named0 = sub_e == routes_ref[0:1, :]
        named1 = sub_e == routes_ref[1:2, :]
        named = named0 | named1
        before = dot(named.astype(F32).astype(BF16), (row < col).astype(F32).astype(BF16))
        rank = jnp.where(named, before, -1.0)
        place = before + ((lax.rem(sub_e, 2) * ep_n + sub_e // 2) * cap).astype(F32)
        slot0 = jnp.sum(jnp.where(named0, place, 0.0), axis=0, keepdims=True)
        slot1 = jnp.sum(jnp.where(named1, place, 0.0), axis=0, keepdims=True)
        stack = jnp.concatenate([slot0, slot1, rw_ref[...], jnp.zeros((4, tokens), F32)], axis=0)
        cols[...] = stack.T

    with jax.named_scope("expert_norm"):
        loads["xin"].wait()
        xf = xin[...].astype(F32)
        factor = lax.rsqrt(jnp.mean(xf * xf, axis=-1, keepdims=True) + NORM_EPSILON)
        mine = []
        for i in range(ns):
            at = pl.ds(pl.multiple_of((4 * i + 2 * par + c) * LANES, LANES), LANES)
            mine.append((xin[:, at].astype(F32) * factor * egain[:, at]).astype(BF16))
        mine = jnp.concatenate(mine, axis=1)
        place_in = lax.broadcasted_iota(jnp.int32, (cap, tokens), 0).astype(F32)

    groups = [pl.ds(0, ns)] if ns == 1 else [pl.ds(0, ns // 2), pl.ds(ns // 2, ns - ns // 2)]
    members = [range(g.start, g.start + g.size) for g in groups]
    mine_rows = pl.ds(pl.multiple_of(ep * cap, 16), cap)

    def dispatch(e):
        group = min(8, ep_n)
        with jax.named_scope("slots"):
            for d0 in range(0, ep_n, group):
                pick = [
                    (place_in == rank[2 * d + e : 2 * d + e + 1, :]).astype(F32).astype(BF16)
                    for d in range(d0, d0 + group)
                ]
                out = dot(jnp.concatenate(pick, axis=0), mine).astype(BF16)
                for d in range(group):
                    for i in range(ns):
                        slots[e, d0 + d, i] = out[d * cap : (d + 1) * cap, i * LANES : (i + 1) * LANES]
        if e == 0:
            with jax.named_scope("barrier"):
                pl.semaphore_wait(barrier, len(peers))
        for g, span in enumerate(groups):
            for k in range(1, ep_n):
                to = lax.rem(ep + k, ep_n)
                there = xbuf.at[e, span, par, c, mine_rows]
                pltpu.make_async_remote_copy(
                    src_ref=slots.at[e, to, span], dst_ref=there, send_sem=a2a_s.at[e, g], recv_sem=a2a_r.at[e, g],
                    device_id=(to, tp), device_id_type=MESH,
                ).start()
        pltpu.make_async_copy(slots.at[e, ep], xbuf.at[e, :, par, c, mine_rows], own_s.at[e]).start()

    axes = (("x", nx, x), ("y", ny, y))

    def ring_to(name, step):
        if name == "x":
            return (y * nx + lax.rem(x + nx + step, nx), tp)
        return (lax.rem(y + ny + step, ny) * nx + x, tp)

    def kv_refs(part, phase, block, j):
        other = (y, x)[part]
        if phase == 0:
            return ktb.at[part, other, block], vb.at[part, other, block]
        n, me = ((nx, x), (ny, y))[part]
        b = lax.rem(me + j, n)
        return ktb.at[part, block, b], vb.at[part, block, b]

    def kv_copies(part, phase, step, j, arriving):
        name, n, me = axes[(part + phase) % 2]
        if n == 1 or step > n // 2:
            return
        tie = 2 * step == n
        for d, sign in ((0, 1), (1, -1)):
            block = lax.rem(me + n - sign * (step if arriving else step - 1), n)
            refs = kv_refs(part, phase, block, j)
            for kind in (0, 1):
                if not tie or kind == d:
                    i = (part, phase * 4 + j, d, step - 1, kind)
                    if arriving:
                        arrived(refs[kind], kvs.at[i], kvr.at[i], ring_to(name, -sign))
                    else:
                        send(refs[kind], refs[kind], kvs.at[i], kvr.at[i], ring_to(name, sign))

    def kv_js(part, step):
        n = (nx, ny)[part]
        return ([0], sorted({1, n - 1} - {0, n}), [2] if n == 4 else [])[step]

    def kv_line(step):
        with jax.named_scope(f"kv_line#s={step}"):
            for part in (0, 1):
                if step:
                    kv_copies(part, 0, step, 0, True)
                kv_copies(part, 0, step + 1, 0, False)
                for j in kv_js(part, step):
                    kv_copies(part, 1, 1, j, False)

    def kv_plane(step, pieces):
        with jax.named_scope(f"kv_plane#s={step}"):
            for part in (0, 1):
                for piece in pieces:
                    for j in kv_js(part, piece):
                        kv_copies(part, 1, step, j, True)
                        kv_copies(part, 1, step + 1, j, False)

    def normed(ref, gain):
        v = ref[...].astype(F32)
        f = lax.rsqrt(jnp.mean(v * v, axis=-1, keepdims=True) + NORM_EPSILON)
        return (v * f * gain[...]).astype(BF16)

    lane = lax.broadcasted_iota(jnp.int32, (tokens, LANES), 1)
    scale = LOG2E * (NOPE + ROPE) ** (-0.5)

    def turned(u):
        left = pltpu.roll(u, LANES - ROPE // 2, 1)
        right = pltpu.roll(u, ROPE // 2, 1)
        other = jnp.where(lax.rem(lane, ROPE) < ROPE // 2, left, right)
        return u * cos_ref[...] + other * sin_ref[...]

    def keys_values():
        with jax.named_scope("kv_proj"):
            for name in ("jl", "wk", "wv"):
                loads[name].wait()
            jn = normed(jl, jgain)
            kt = dot(jn, wk[...]).T.astype(BF16)
            wide = jnp.concatenate([rk_ref[...].astype(F32), jnp.zeros((LANES - ROPE, tokens), F32)], axis=0)
            rt = turned(wide.T).T[0:ROPE].astype(BF16)
            vv = dot(jn, wv[...]).astype(BF16)
            for h, (a, b) in enumerate(((y, x), (x, y))):
                part = slice(h * half, (h + 1) * half)
                ktb[h, a, b, 0:NOPE, :] = kt[0:NOPE, part]
                ktb[h, a, b, NOPE : NOPE + ROPE, :] = rt[:, part]
                ktb[h, a, b, NOPE + ROPE :, :] = kt[NOPE:, part]
                vb[h, a, b] = vv[part]
        kv_line(0)

    def queries():
        with jax.named_scope("q_proj"):
            for name in ("ql", "wq", "wr"):
                loads[name].wait()
            qn = normed(ql, qgain)
            plain = dot(qn, wq[...])
            rope = dot_nt(qn, wr[...])
            rope = turned(jnp.concatenate([rope, jnp.zeros((tokens, LANES - 2 * ROPE), F32)], axis=1))
            first = jnp.where(lane < NOPE, plain, jnp.where(lane < NOPE + ROPE, pltpu.roll(rope, NOPE, 1), 0.0))
            second = jnp.where(lane < ROPE, 0.0, jnp.where(lane < NOPE, rope, plain))
            q_s[0] = (first * scale).astype(BF16)
            q_s[1] = (second * scale).astype(BF16)

    def a2a_wait(e, g):
        if g >= len(groups):
            return
        span = groups[g]
        with jax.named_scope(f"a2a_wait#e={e}#g={g}"):
            if g == 0:
                pltpu.make_async_copy(slots.at[e, ep], xbuf.at[e, :, par, c, mine_rows], own_s.at[e]).wait()
            both = pltpu.make_async_remote_copy(
                src_ref=slots.at[e, pl.ds(0, ep_n - 1), span], dst_ref=xbuf.at[e, span, par, c, pl.ds(0, rows - cap)],
                send_sem=a2a_s.at[e, g], recv_sem=a2a_r.at[e, g], device_id=sib, device_id_type=MESH,
            )
            both.wait_recv()
            pending.append(both)
        for i in members[g]:
            piece = xbuf.at[e, i, par, c]
            send(piece, piece, zs.at[e, i], zr.at[e, i], z_to[i % 2])
        piece = xbuf.at[e, span, par, c]
        send(piece, piece, dds.at[e, ns + g], ddr.at[e, ns + g], sib)

    def z_wait(e, g):
        if g >= len(groups):
            return
        with jax.named_scope(f"z_wait#e={e}#g={g}"):
            for i in members[g]:
                piece = xbuf.at[e, i, opar, c]
                arrived(piece, zs.at[e, i], zr.at[e, i], z_to[1 - i % 2])
                send(piece, piece, dds.at[e, i], ddr.at[e, i], sib)

    row_tile = 256 if rows % 256 == 0 else rows // 2

    def pair_copy(e, t):
        at = pl.ds(pl.multiple_of(t * row_tile, row_tile), row_tile)
        return pltpu.make_async_remote_copy(
            src_ref=pbuf.at[e, :, oc, at], dst_ref=sbuf.at[e, :, at], send_sem=pss.at[e, t], recv_sem=psr.at[e, t],
            device_id=sib, device_id_type=MESH,
        )

    def expert(e):
        with jax.named_scope(f"dd_wait#e={e}"):
            for g, span in enumerate(groups):
                arrived(xbuf.at[e, span, par, oc], dds.at[e, ns + g], ddr.at[e, ns + g], sib)
            for i in range(ns):
                arrived(xbuf.at[e, i, opar, oc], dds.at[e, i], ddr.at[e, i], sib)

        def tile(t, carry):
            at = pl.ds(pl.multiple_of(t * row_tile, row_tile), row_tile)
            xx = jnp.concatenate([xbuf[e, j // 4, j // 2 % 2, j % 2, at] for j in range(2 * nz)], axis=1)
            gate = dot(xx, wg[e])
            up = dot(xx, wu[e])
            hidden = (gate / (1.0 + jnp.exp(-gate)) * up).astype(BF16)
            part = dot(hidden, wd[e]).astype(BF16)
            for j in range(2 * nz):
                pbuf[e, j // 2, j % 2, at] = part[:, j * LANES : (j + 1) * LANES]
            pair_copy(e, t).start()
            return carry

        with jax.named_scope(f"expert#e={e}"):
            lax.fori_loop(0, rows // row_tile, tile, 0)
        for t in range(rows // row_tile):
            pending.append(pair_copy(e, t))

    hz = nz // 2

    def reducer(name, p, s, r, t, ssem, rsem):
        cut = p.shape[2] // 2

        def term(dest, at):
            return p[dest, c, at].astype(F32) + s[dest, at].astype(F32)

        def put(own, step):
            if step > hz:
                return
            for d, sign in ((0, 1), (1, -1)):
                g = d if own else 1 - d
                at = pl.ds(g * cut, cut)
                dest = lax.rem(z + sign * (hz + 1 - step) + nz, nz)
                v = term(dest, at)
                if step > (1 if own else 2):
                    v = v + r[d, step - 2, at].astype(F32)
                t[d, step - 1, at] = v.astype(BF16)
                i = (d, g, step - 1)
                send(t.at[d, step - 1, at], r.at[d, step - 1, at], ssem.at[i], rsem.at[i], z_to[d])

        def take(own, step):
            for d in (0, 1):
                g = d if own else 1 - d
                at = pl.ds(g * cut, cut)
                i = (d, g, step - 1)
                arrived(r.at[d, step - 1, at], ssem.at[i], rsem.at[i], z_to[1 - d])

        events = []
        for step in range(1, hz + 1):
            events.append((True, step))
            if step < hz:
                events.append((False, step + 1))

        def start():
            with jax.named_scope(f"start#{name}"):
                put(True, 1)
                put(False, 2)

        def event():
            own, step = events.pop(0)
            with jax.named_scope(f"take#{name}#own={int(own)}#s={step}"):
                take(own, step)
            put(own, step + 1)

        def last():
            out = []
            for g in (0, 1):
                at = pl.ds(g * cut, cut)
                v = term(z, at)
                for d in (0, 1):
                    if hz > 1 or g == d:
                        v = v + r[d, hz - 1, at].astype(F32)
                out.append(v.astype(BF16))
            return out

        return start, event, last, events

    hr = rows // 2

    def finish(e, last):
        with jax.named_scope(f"finish#e={e}"):
            for g, v in enumerate(last()):
                fin[e, g * hr : (g + 1) * hr] = v
            for k in range(1, ep_n):
                to = lax.rem(ep + k, ep_n)
                src = fin.at[e, pl.ds(pl.multiple_of(to * cap, 16), cap)]
                pltpu.make_async_remote_copy(
                    src_ref=src, dst_ref=ret.at[e, ep], send_sem=bks.at[e], recv_sem=bkr.at[e],
                    device_id=(to, tp), device_id_type=MESH,
                ).start()
            ret[e, ep] = fin[e, mine_rows]

    q_tile = min(256, tokens)

    def unit(part, a):
        blocks = (nx, ny)[part]

        def tile(t):
            at = pl.ds(t * q_tile, q_tile)
            both = []
            for head in (0, 1):
                q = q_s[head, at]
                both.append([dot(q, ktb[part, a, b, head * ROPE : head * ROPE + LANES, :]) for b in range(blocks)])
            vals = jnp.concatenate([vb[part, a, b] for b in range(blocks)], axis=0)
            for head, s in enumerate(both):
                m_old = m_s[head, at]
                m_new = jnp.maximum(m_old, jnp.max(functools.reduce(jnp.maximum, s), axis=1, keepdims=True))
                alpha = jnp.exp2(m_old - m_new)
                m_s[head, at] = m_new
                p = [jnp.exp2(v[:, i : i + LANES] - m_new) for v in s for i in range(0, half, LANES)]
                l_s[head, at] = l_s[head, at] * alpha + functools.reduce(jnp.add, p)
                p = jnp.concatenate([v.astype(BF16) for v in p], axis=1)
                acc_s[head, at] = acc_s[head, at] * alpha + dot(p, vals)

        return tile

    a0 = (y, x)
    alen = (ny, nx)
    tiles = tokens // q_tile
    todo = []
    for near in ((0,), (1, 2), (3,)):
        pairs = [(part, i) for i in near for part in (0, 1) if i < alen[part]]
        if near == (3,) or max(alen) < 4:
            todo += [(part, i, t) for t in range(tiles) for part, i in pairs]
        else:
            todo += [(part, i, t) for part, i in pairs for t in range(tiles)]

    def some(count=1):
        for _ in range(count):
            if todo:
                part, i, t = todo.pop(0)
                off = (0, alen[part] - 1, 1, 2)[i] if alen[part] > 2 else i
                with jax.named_scope(f"unit#n={len(todo)}"):
                    unit(part, lax.rem(a0[part] + off, alen[part]))(t)

    red = [
        reducer(f"e{e}", pbuf.at[e], sbuf.at[e], rbuf.at[e], tbuf.at[e], rss.at[e], rsr.at[e]) for e in (0, 1)
    ]

    def pair(e):
        with jax.named_scope(f"pair#e={e}"):
            for t in range(rows // row_tile):
                pair_copy(e, t).wait_recv()

    def out_proj():
        with jax.named_scope("out_proj"):
            loads["wo"].wait()
            t0 = jnp.sum(l_s[0], axis=1, keepdims=True)
            t1 = jnp.sum(l_s[1], axis=1, keepdims=True)
            attended = jnp.where(lane < VDIM, acc_s[0] / t0, acc_s[1] / t1).astype(BF16)
            per = tokens // (2 * nz)
            for q in range(0, nz, hz):
                proj = dot(attended[q * 2 * per : (q + hz) * 2 * per], wo[...]).astype(BF16)
                for i in range(2 * hz):
                    ap[q + i // 2, i % 2] = proj[i * per : (i + 1) * per]
                span = pl.ds(q, hz)
                send(ap.at[span, oc], asb.at[span], aps.at[q // hz], apr.at[q // hz], sib)

    def combine():
        with jax.named_scope("combine_wait"):
            for e in (0, 1):
                both = pltpu.make_async_remote_copy(
                    src_ref=fin.at[e, pl.ds(0, rows - cap)], dst_ref=ret.at[e, pl.ds(0, ep_n - 1)],
                    send_sem=bks.at[e], recv_sem=bkr.at[e], device_id=sib, device_id_type=MESH,
                )
                both.wait_recv()
                pending.append(both)
        with jax.named_scope("combine"):
            slot_count = experts * cap
            where_at = lax.broadcasted_iota(jnp.int32, (tokens, slot_count), 1).astype(F32)
            rets = ret[...].reshape(slot_count, LANES)
            total = jnp.zeros((tokens, LANES), F32)
            for k in (0, 1):
                pick = (where_at == cols[:, k : k + 1]).astype(F32).astype(BF16)
                total = total + dot(pick, rets) * cols[:, 2 + k : 3 + k]
            expert_ref[...] = total.astype(BF16)

    red.append(reducer("a", ap, asb, arb, atb, ars, arr))

    def step_of(e):
        if red[e][3]:
            red[e][1]()
            if e < 2 and not red[e][3]:
                finish(e, red[e][2])

    kv_state = []

    def kv_upto(count):
        for stage in range(len(kv_state) + 1, count + 1):
            kv_state.append(stage)
            if stage == 1:
                kv_plane(1, (0, 1))
            elif stage == 2:
                kv_plane(1, (2,))
            else:
                kv_plane(2, (0, 1, 2))

    def work(count):
        for _ in range(count):
            if not todo:
                return
            if len(todo) <= 6 * tiles:
                kv_upto(2)
            if len(todo) <= 2 * tiles:
                kv_upto(3)
            some()

    dispatch(0)
    dispatch(1)
    keys_values()
    m_s[...] = jnp.full(m_s.shape, -jnp.inf, F32)
    l_s[...] = jnp.zeros(l_s.shape, F32)
    acc_s[...] = jnp.zeros(acc_s.shape, F32)
    queries()
    a2a_wait(0, 0)
    a2a_wait(0, 1)
    z_wait(0, 0)
    a2a_wait(1, 0)
    z_wait(0, 1)
    a2a_wait(1, 1)
    for name in ("wg", "wu", "wd"):
        loads[name].wait()
    expert(0)
    kv_line(1)
    z_wait(1, 0)
    pair(0)
    red[0][0]()
    z_wait(1, 1)
    expert(1)
    step_of(0)
    pair(1)
    red[1][0]()
    kv_line(2)
    work(1)
    step_of(0)
    work(3)
    step_of(0)
    flush(60)
    step_of(1)
    kv_upto(1)
    kv_upto(2)
    work(2)
    step_of(1)
    work(3)
    step_of(0)
    work(2)
    step_of(0)
    work(2)
    step_of(1)
    work(len(todo))
    out_proj()
    step_of(1)
    step_of(0)
    with jax.named_scope("pair#a"):
        for q in range(0, nz, hz):
            arrived(asb.at[pl.ds(q, hz)], aps.at[q // hz], apr.at[q // hz], sib)
    red[2][0]()
    step_of(0)
    flush(50)
    step_of(1)
    step_of(1)
    step_of(2)
    step_of(2)
    step_of(1)
    for e in (0, 1):
        while red[e][3]:
            step_of(e)
    flush(40)
    for _ in range(3):
        step_of(2)
    combine()
    flush(len(pending) - 2)
    while red[2][3]:
        step_of(2)
    cut = mixer_ref.shape[0] // 2
    for g, v in enumerate(red[2][2]()):
        mixer_ref[g * cut : (g + 1) * cut] = v

    flush(len(pending))


def back_kernel(mixer, expert, mixer_out, expert_out):
    mixer_out[...] = mixer[...]
    expert_out[...] = expert[...]


def rotary_tables(tokens):
    half_width = ROPE // 2
    positions = (lax.axis_index("ep") * tokens + jnp.arange(tokens, dtype=jnp.int32)).astype(F32)
    lanes = jnp.arange(LANES, dtype=jnp.int32) % ROPE
    frequencies = ROTARY_BASE ** (-(lanes % half_width).astype(F32) / half_width)
    angles = positions[:, None] * frequencies[None, :]
    sine = jnp.sin(angles)
    return jnp.cos(angles), jnp.where(lanes[None, :] < half_width, -sine, sine)


def local(
    dims,
    query_latent, joint_latent, rotary_key, query_gain, joint_gain, query_weight, query_rotary,
    key_weight, value_weight, output_weight, expert_input, expert_gain, routes, route_weight,
    gate_weight, up_weight, down_weight,
):
    ny, nx, nz = dims
    ep_n, tokens, width = ny * nx, query_latent.shape[0], output_weight.shape[1]
    cap = 3 * tokens // (2 * ep_n)
    rows = ep_n * cap
    half = tokens // 2
    cos, sin = rotary_tables(tokens)

    hz = nz // 2
    per = tokens // (2 * nz)
    sds = jax.ShapeDtypeStruct
    vmem = pl.BlockSpec(memory_space=pltpu.VMEM)
    hbm = pl.BlockSpec(memory_space=pl.ANY)
    sem = pltpu.SemaphoreType.DMA
    side = max(ny, nx)
    streamed = [
        expert_input, joint_latent, key_weight, value_weight, query_latent, query_weight, query_rotary.T,
        gate_weight, up_weight, down_weight, output_weight,
    ]
    scratch = [pltpu.VMEM(a.shape, a.dtype) for a in streamed] + [
        pltpu.VMEM((2, ep_n, hz, cap, LANES), BF16),
        pltpu.VMEM((2, hz, 2, 2, rows, LANES), BF16),
        pltpu.VMEM((2, nz, 2, rows, LANES), BF16),
        pltpu.VMEM((2, nz, rows, LANES), BF16),
        pltpu.VMEM((2, 2, hz, rows, LANES), BF16),
        pltpu.VMEM((2, 2, hz, rows, LANES), BF16),
        pltpu.VMEM((2, rows, LANES), BF16),
        pltpu.VMEM((2, ep_n, cap, LANES), BF16),
        pltpu.VMEM((2, side, side, LANES + ROPE, half), BF16),
        pltpu.VMEM((2, side, side, half, LANES), BF16),
        pltpu.VMEM((2, tokens, LANES), BF16),
        pltpu.VMEM((tokens, 8), F32),
        pltpu.VMEM((2, tokens, LANES), F32),
        pltpu.VMEM((2, tokens, LANES), F32),
        pltpu.VMEM((2, tokens, LANES), F32),
        pltpu.VMEM((nz, 2, per, width), BF16),
        pltpu.VMEM((nz, per, width), BF16),
        pltpu.VMEM((2, hz, per, width), BF16),
        pltpu.VMEM((2, hz, per, width), BF16),
        sem((2, 2)), sem((2, 2)),
        sem((2, hz)), sem((2, hz)),
        sem((2, hz + 2)), sem((2, hz + 2)),
        sem((2, 8, 2, 2, 2)), sem((2, 8, 2, 2, 2)),
        sem((2, 4)), sem((2, 4)),
        sem((2, 2, 2, hz)), sem((2, 2, 2, hz)),
        sem((2,)), sem((2,)),
        sem((2,)), sem((2,)),
        sem((2, 2, hz)), sem((2, 2, hz)),
        sem((len(streamed),)),
        sem((2,)),
    ]
    mixer, expert = pl.pallas_call(
        functools.partial(main_kernel, (ny, nx, nz, cap)),
        out_shape=(sds((per, width), BF16), sds((tokens, LANES), BF16)),
        in_specs=[vmem] * 8 + [hbm] * len(streamed),
        out_specs=(vmem, vmem),
        scratch_shapes=scratch,
        compiler_params=pltpu.CompilerParams(
            collective_id=0, has_side_effects=True, vmem_limit_bytes=62 * 2**20
        ),
        name="main",
    )(
        routes.T, route_weight.T, query_gain[None], joint_gain[None], expert_gain[None], rotary_key.T, cos, sin,
        *streamed,
    )
    return pl.pallas_call(
        back_kernel,
        out_shape=(sds(mixer.shape, BF16), sds(expert.shape, BF16)),
        name="back",
    )(mixer, expert)


def solution(mesh):
    ny, nx = ep_grid(mesh.shape["ep"])
    return jax.shard_map(
        functools.partial(local, (ny, nx, mesh.shape["tp"] // 2)),
        mesh=mesh,
        in_specs=(
            P("ep", None),
            P("ep", None),
            P("ep", None),
            P(),
            P(),
            P(None, "tp"),
            P(None, "tp"),
            P(None, "tp"),
            P(None, "tp"),
            P("tp", None),
            P("ep", None),
            P(),
            P("ep", None),
            P("ep", None),
            P("ep", None, "tp"),
            P("ep", None, "tp"),
            P("ep", "tp", None),
        ),
        out_specs=(P(("ep", "tp"), None), P("ep", "tp")),
        check_vma=False,
    )
```
